32 devices in a mesh: sp: 8 (over z, x), tp: 4 (over y, core).
Axes of the slice: x: 2, y: 2, z: 4, core: 2. Of those that a mesh axis runs over, the one named last changes fastest.
Arguments:
- query_wide: bfloat16 [1024, 1536], P('sp', 'tp'), may hold values from -600 to 600
- query_narrow: bfloat16 [1024, 1024], P('sp', 'tp'), may hold values from -600 to 600
- latent: bfloat16 [1024, 512], P('sp'), may hold values from -6 to 6
- rope_key: bfloat16 [1024, 64], P('sp'), may hold values from -6 to 6
- latent_norm_weight: float32 [512], replicated, may hold values from 0.1 to 1.9
- broad_key_lift: bfloat16 [512, 1024], P(None, 'tp'), may hold values from -0.25 to 0.25
- broad_value_lift: bfloat16 [512, 1024], P(None, 'tp'), may hold values from -0.25 to 0.25
- slim_key_lift: bfloat16 [512, 512], P(None, 'tp'), may hold values from -0.25 to 0.25
- slim_value_lift: bfloat16 [512, 512], P(None, 'tp'), may hold values from -0.25 to 0.25
- out_wide: bfloat16 [1024, 2048], P('tp'), may hold values from -0.4375 to 0.4375
- out_narrow: bfloat16 [512, 2048], P('tp'), may hold values from -0.4375 to 0.4375
- resid: bfloat16 [1024, 2048], P('sp'), may hold values from -20 to 20
- ffn_gain: float32 [2048], replicated, may hold values from 0.1 to 1.9
- group_route: int32 [1024], P('sp'), may hold values from 0 to 7, as said below
- expert_pair: int32 [1024, 2], P('sp'), may hold values from 0 to 3, all different within a row
- group_prob: float32 [1024], P('sp'), may hold values from 0.2 to 1
- expert_prob: float32 [1024, 2], P('sp'), may hold values from 0.05 to 1
- gate_weight: bfloat16 [8, 4, 2048, 512], P('sp', None, None, 'tp'), may hold values from -0.125 to 0.125
- up_weight: bfloat16 [8, 4, 2048, 512], P('sp', None, None, 'tp'), may hold values from -0.125 to 0.125
- down_weight: bfloat16 [8, 4, 512, 2048], P('sp', None, 'tp'), may hold values from -0.25 to 0.25
Outputs:
- mixed: bfloat16 [1024, 2048], P('sp', 'tp')
The draws below stay inside these ranges and needn't reach their ends.
Inputs may be any that keep to these rules, and one draw needn't show every extreme that they name: `group_route`: of the 128 tokens of one index of sp at most 32 name one group; in every draw one group is named by exactly 32 tokens of every index of sp, and every index of sp names one more group exactly 32 times. `expert_pair`: A token's two experts are different.
All inputs are finite; a program needn't handle non-finite values.
Results may differ from the reference program's by a relative error of at most 0.017.
Values may be sent and summed in bfloat16 or wider, within the bound.
A program may use at most 128 MiB of HBM per device.

```python
import math
import jax
import jax.numpy as jnp
from jax import lax

D = 2048
WIDE_HEADS = 8
SLIM_HEADS = 8
PLAIN_WIDTH_WIDE = 128
PLAIN_WIDTH_SLIM = 64
ROPE = 64
VALUE_WIDTH_WIDE = 128
VALUE_WIDTH_SLIM = 64
LATENT_RANK = 512
EPG = 4
FF = 512
TOK_DEV = 128
TOKEN_COUNT = 1024
GROUPS = 8
CAP = 32
N_SP = 8
N_TP = 4


def query_draw(key, columns):
    base_values = 2.5 * jax.random.truncated_normal(key, -6.0, 6.0, (TOKEN_COUNT, columns), jnp.float32)
    return base_values.astype(jnp.bfloat16)


def draw_query_wide(key, part):
    return query_draw(jax.random.fold_in(key, 3), WIDE_HEADS * (PLAIN_WIDTH_WIDE + ROPE))


def draw_query_narrow(key, part):
    return query_draw(jax.random.fold_in(key, 5), SLIM_HEADS * (PLAIN_WIDTH_SLIM + ROPE))


def draw_resid(key, part):
    column = jnp.arange(D).astype(jnp.float32)
    column_scale = 0.3 * 9.0 ** (column / (D - 1))
    base_values = jax.random.truncated_normal(jax.random.fold_in(key, 19), -6.0, 6.0, (TOKEN_COUNT, D), jnp.float32)
    return (base_values * column_scale[None, :]).astype(jnp.bfloat16)


def draw_group_route(key, part):
    heavy_all = jax.random.randint(jax.random.fold_in(key, 11), (), 0, GROUPS)
    slot_group = (jnp.arange(GROUPS * CAP) // CAP).astype(jnp.int32)

    def one_device(device_index):
        device_key = jax.random.fold_in(jax.random.fold_in(key, 13), device_index)
        first_key, second_key, third_key = jax.random.split(device_key, 3)
        second_group = (heavy_all + 1 + jax.random.randint(first_key, (), 0, GROUPS - 1)) % GROUPS
        shuffled = jax.random.permutation(second_key, GROUPS * CAP)
        position = jnp.zeros((GROUPS * CAP,), jnp.int32).at[shuffled].set(jnp.arange(GROUPS * CAP, dtype=jnp.int32))
        heavy_slot = (slot_group == heavy_all) | (slot_group == second_group)
        sort_score = jnp.where(heavy_slot, jnp.arange(GROUPS * CAP, dtype=jnp.int32), GROUPS * CAP + position)
        picked = slot_group[jnp.argsort(sort_score, stable=True)][:TOK_DEV]
        return picked[jax.random.permutation(third_key, TOK_DEV)]
    return jax.vmap(one_device)(jnp.arange(GROUPS)).reshape(TOKEN_COUNT).astype(jnp.int32)


def level_of(own_key, dims, cuts, low, high):
    gain = 1.0
    for axis_at, blocks in cuts:
        steps = jax.random.uniform(jax.random.fold_in(jax.random.fold_in(own_key, 6), axis_at), (blocks,), jnp.float32, low / len(cuts), high / len(cuts))
        gain = gain * jnp.repeat(jnp.exp(steps), dims[axis_at] // blocks).reshape((-1,) + (1,) * (len(dims) - 1 - axis_at))
    return gain


def choose_distinct(own_key, rows, number_of, top, lift):
    sequence = jax.random.permutation(jax.random.fold_in(own_key, 1), number_of)
    favour = sequence
    for power in range(3):
        favour = favour * favour // number_of
    favour = favour * lift // number_of
    lots = jax.random.randint(jax.random.fold_in(own_key, 2), (rows, number_of), 0, 4096) + favour
    holders = jax.random.permutation(jax.random.fold_in(own_key, 3), rows)[jnp.arange(number_of) % rows]
    lots = jnp.where(jnp.arange(rows)[:, None] == holders[None, :], 1 << 14, lots)
    priority = lots * number_of + jnp.arange(number_of)
    return lax.top_k(priority.astype(jnp.int32), top)[1].astype(jnp.int32)


def noise(rng, extent, scale, bound, pieces=(), held_as=jnp.bfloat16):
    factor_of = level_of(rng, extent, pieces, -0.22, 0.18) if pieces else 1.0
    result = jax.random.normal(rng, extent, jnp.float32) * scale * factor_of
    return jnp.minimum(jnp.maximum(result, -bound), bound).astype(held_as)


def setup_inputs(seed: int = 0) -> dict:
    seeds = jax.random.split(jax.random.key(seed), 21)
    return {
        "query_wide": draw_query_wide(jax.random.fold_in(seeds[20], 71), 0),
        "query_narrow": draw_query_narrow(jax.random.fold_in(seeds[20], 71), 0),
        "latent": noise(seeds[2], (TOKEN_COUNT, LATENT_RANK), 1.0, 6.0, ((0, 8),)),
        "rope_key": noise(seeds[3], (TOKEN_COUNT, ROPE), 1.0, 6.0, ((0, 8),)),
        "latent_norm_weight": jnp.clip(1.0 + 0.18 * jax.random.normal(seeds[4], (LATENT_RANK,), jnp.float32), 0.1, 1.9),
        "broad_key_lift": noise(seeds[5], (LATENT_RANK, WIDE_HEADS * PLAIN_WIDTH_WIDE), LATENT_RANK ** -0.5, 0.25, ((1, 4),)),
        "broad_value_lift": noise(seeds[6], (LATENT_RANK, WIDE_HEADS * VALUE_WIDTH_WIDE), LATENT_RANK ** -0.5, 0.25, ((1, 4),)),
        "slim_key_lift": noise(seeds[7], (LATENT_RANK, SLIM_HEADS * PLAIN_WIDTH_SLIM), LATENT_RANK ** -0.5, 0.25, ((1, 4),)),
        "slim_value_lift": noise(seeds[8], (LATENT_RANK, SLIM_HEADS * VALUE_WIDTH_SLIM), LATENT_RANK ** -0.5, 0.25, ((1, 4),)),
        "out_wide": noise(seeds[9], (WIDE_HEADS * VALUE_WIDTH_WIDE, D), ((WIDE_HEADS * VALUE_WIDTH_WIDE + SLIM_HEADS * VALUE_WIDTH_SLIM) // 9) ** -0.5, 0.4375, ((0, 4),)),
        "out_narrow": noise(seeds[10], (SLIM_HEADS * VALUE_WIDTH_SLIM, D), ((WIDE_HEADS * VALUE_WIDTH_WIDE + SLIM_HEADS * VALUE_WIDTH_SLIM) // 9) ** -0.5, 0.4375, ((0, 4),)),
        "resid": draw_resid(jax.random.fold_in(seeds[20], 71), 0),
        "ffn_gain": jnp.clip(1.0 + 0.18 * jax.random.normal(seeds[12], (D,), jnp.float32), 0.1, 1.9),
        "group_route": draw_group_route(jax.random.fold_in(seeds[20], 71), 0),
        "expert_pair": choose_distinct(seeds[14], TOKEN_COUNT, EPG, 2, 0),
        "group_prob": jnp.clip(0.2 + 0.8 * jax.random.uniform(seeds[15], (TOKEN_COUNT,), jnp.float32) ** level_of(seeds[15], (TOKEN_COUNT,), ((0, 8),), -0.2, 0.2), 0.2, 1.0),
        "expert_prob": jnp.clip(jnp.exp(math.log(1.0) - 2.9957323 * jax.random.uniform(seeds[16], (TOKEN_COUNT, 2), jnp.float32) ** level_of(seeds[16], (TOKEN_COUNT, 2), ((0, 8),), -0.2, 0.2)), 0.05, 1.0),
        "gate_weight": noise(seeds[17], (GROUPS, EPG, D, FF), D ** -0.5, 0.125, ((0, 8), (3, 4))),
        "up_weight": noise(seeds[18], (GROUPS, EPG, D, FF), D ** -0.5, 0.125, ((0, 8), (3, 4))),
        "down_weight": noise(seeds[19], (GROUPS, EPG, FF, D), FF ** -0.5, 0.25, ((0, 8), (2, 4))),
    }


ROPE_BASE = 10000.0
EPSILON = 1e-06

def rms_scale(values, gain_row):
    widened = values.astype(jnp.float32)
    return widened * lax.rsqrt(lax.optimization_barrier(jnp.mean(widened * widened, axis=-1, keepdims=True)) + EPSILON) * gain_row.astype(jnp.float32)

def angles(positions, width):
    frequency = 1.0 / ROPE_BASE ** (jnp.arange(0, width, 2).astype(jnp.float32) / width)
    return positions.astype(jnp.float32)[:, None] * frequency[None, :]

def rotary(values, angle_table):
    half_width = values.shape[-1] // 2
    first_half = values[..., :half_width]
    second = values[..., half_width:]
    return jnp.concatenate([first_half * jnp.cos(angle_table) - second * jnp.sin(angle_table), second * jnp.cos(angle_table) + first_half * jnp.sin(angle_table)], axis=-1)

def stored(values):
    return lax.optimization_barrier(values.astype(jnp.bfloat16)).astype(jnp.float32)

def attention(query_nope, query_rot, key_nope, key_rot, value_rows, scale):
    key_pos = jnp.arange(TOKEN_COUNT).astype(jnp.int32)

    def one_block(block_index):
        first_row = (block_index * TOK_DEV).astype(jnp.int32)
        nope_rows = lax.dynamic_slice_in_dim(query_nope, first_row, TOK_DEV, 0)
        rot_rows = lax.dynamic_slice_in_dim(query_rot, first_row, TOK_DEV, 0)
        scores = jnp.einsum('thd,khd->htk', nope_rows, key_nope) + jnp.einsum('thd,kd->htk', rot_rows, key_rot)
        scores = scores * scale
        query_pos = first_row + jnp.arange(TOK_DEV).astype(jnp.int32)
        scores = jnp.where((query_pos[:, None] >= key_pos[None, :])[None], scores, -jnp.inf)
        row_peak = lax.optimization_barrier(jnp.max(scores, axis=-1, keepdims=True))
        weights = jnp.exp(scores - row_peak)
        row_total = lax.optimization_barrier(jnp.sum(weights, axis=-1))
        mixed_rows = jnp.einsum('htk,khd->thd', stored(weights), value_rows)
        return (mixed_rows / row_total.T[:, :, None]).astype(jnp.bfloat16)
    blocks = lax.map(one_block, jnp.arange(TOKEN_COUNT // TOK_DEV).astype(jnp.int32))
    return blocks.reshape(TOKEN_COUNT, -1)

def reference(query_wide, query_narrow, latent, rope_key, latent_norm_weight, broad_key_lift, broad_value_lift, slim_key_lift, slim_value_lift, out_wide, out_narrow, resid, ffn_gain, group_route, expert_pair, group_prob, expert_prob, gate_weight, up_weight, down_weight):
    angle_table = angles(jnp.arange(TOKEN_COUNT).astype(jnp.int32), ROPE)
    latent_rows = rms_scale(latent, latent_norm_weight).astype(jnp.bfloat16)
    key_rot = stored(rotary(rope_key.astype(jnp.float32), angle_table))
    key_wide = stored(jnp.dot(latent_rows, broad_key_lift, preferred_element_type=jnp.float32)).reshape(TOKEN_COUNT, WIDE_HEADS, PLAIN_WIDTH_WIDE)
    value_wide = stored(jnp.dot(latent_rows, broad_value_lift, preferred_element_type=jnp.float32)).reshape(TOKEN_COUNT, WIDE_HEADS, VALUE_WIDTH_WIDE)
    key_narrow = stored(jnp.dot(latent_rows, slim_key_lift, preferred_element_type=jnp.float32)).reshape(TOKEN_COUNT, SLIM_HEADS, PLAIN_WIDTH_SLIM)
    value_narrow = stored(jnp.dot(latent_rows, slim_value_lift, preferred_element_type=jnp.float32)).reshape(TOKEN_COUNT, SLIM_HEADS, VALUE_WIDTH_SLIM)
    wide_rows = query_wide.reshape(TOKEN_COUNT, WIDE_HEADS, PLAIN_WIDTH_WIDE + ROPE).astype(jnp.float32)
    wide_rot = stored(rotary(wide_rows[..., PLAIN_WIDTH_WIDE:], angle_table[:, None, :]))
    narrow_rows = query_narrow.reshape(TOKEN_COUNT, SLIM_HEADS, PLAIN_WIDTH_SLIM + ROPE).astype(jnp.float32)
    narrow_rot = stored(rotary(narrow_rows[..., PLAIN_WIDTH_SLIM:], angle_table[:, None, :]))
    att_wide = attention(wide_rows[..., :PLAIN_WIDTH_WIDE], wide_rot, key_wide, key_rot, value_wide, (PLAIN_WIDTH_WIDE + ROPE) ** (-0.5))
    att_narrow = attention(narrow_rows[..., :PLAIN_WIDTH_SLIM], narrow_rot, key_narrow, key_rot, value_narrow, (PLAIN_WIDTH_SLIM + ROPE) ** (-0.5))
    wide_share = WIDE_HEADS // N_TP * VALUE_WIDTH_WIDE
    narrow_share = SLIM_HEADS // N_TP * VALUE_WIDTH_SLIM
    projected = jnp.zeros((TOKEN_COUNT, D), jnp.float32)
    for part_index in range(N_TP):
        wide_lo = part_index * wide_share
        narrow_lo = part_index * narrow_share
        partial_value = jnp.dot(att_wide[:, wide_lo:wide_lo + wide_share], out_wide[wide_lo:wide_lo + wide_share], preferred_element_type=jnp.float32)
        partial_value = partial_value + jnp.dot(att_narrow[:, narrow_lo:narrow_lo + narrow_share], out_narrow[narrow_lo:narrow_lo + narrow_share], preferred_element_type=jnp.float32)
        projected = projected + stored(partial_value)
    stream = (resid.astype(jnp.float32) + projected).astype(jnp.bfloat16)
    normed = rms_scale(stream, ffn_gain).astype(jnp.bfloat16)
    share_of = group_prob[:, None] * expert_prob / lax.optimization_barrier(jnp.sum(expert_prob, axis=1, keepdims=True))
    chosen = (expert_pair[:, :, None] == jnp.arange(EPG).astype(jnp.int32)[None, None, :]).astype(jnp.float32)
    combine = lax.optimization_barrier(jnp.sum(share_of[:, :, None] * chosen, axis=1)).astype(jnp.bfloat16)
    slot_count = N_SP * CAP
    member = (group_route[:, None] == jnp.arange(GROUPS).astype(jnp.int32)[None, :]).astype(jnp.int32)
    group_rank = lax.optimization_barrier(jnp.sum(jnp.cumsum(member, axis=0) * member, axis=1)) - 1
    slot_index = (group_route * slot_count + group_rank).astype(jnp.int32)
    routed_rows = jnp.zeros((GROUPS * slot_count, D), jnp.bfloat16).at[slot_index].set(normed)
    routed_weights = jnp.zeros((GROUPS * slot_count, EPG), jnp.bfloat16).at[slot_index].set(combine)

    def one_group(operands):
        group_rows, group_weights, gate_group, up_group, down_group = operands
        flat_rows = stored(group_rows)
        gate_act = jnp.einsum('rd,edf->ref', flat_rows, gate_group.astype(jnp.float32))
        up_act = jnp.einsum('rd,edf->ref', flat_rows, up_group.astype(jnp.float32))
        hidden = stored(jax.nn.silu(gate_act) * up_act * group_weights.astype(jnp.float32)[:, :, None])
        hidden = hidden.reshape(slot_count, EPG, N_TP, FF // N_TP)
        down_split = down_group.astype(jnp.float32).reshape(EPG, N_TP, FF // N_TP, D)
        partials = stored(jnp.einsum('repf,epfd->prd', hidden, down_split))
        return lax.optimization_barrier(jnp.sum(partials, axis=0)).astype(jnp.bfloat16)
    results = lax.map(one_group, (routed_rows.reshape(GROUPS, slot_count, D), routed_weights.reshape(GROUPS, slot_count, EPG), gate_weight, up_weight, down_weight))
    moe = results.reshape(GROUPS * slot_count, D)[slot_index]
    return (stream.astype(jnp.float32) + moe.astype(jnp.float32)).astype(jnp.bfloat16)
```

```python
import functools

import jax
import jax.numpy as jnp
import numpy as np
from jax import lax
from jax.experimental import pallas as pl
from jax.experimental.pallas import tpu as pltpu
from jax.sharding import PartitionSpec as P

PLAIN_WIDE = 128
PLAIN_SLIM = 64
ROPE = 64
LANES = 128
ROPE_BASE = 10000.0
EPSILON = 1e-06
MASKED = -1e30
F32 = jnp.float32
BF16 = jnp.bfloat16
MESH = pl.DeviceIdType.MESH


def dot(a, b):
    return jnp.dot(a, b, preferred_element_type=F32)


def dot_nt(a, b):
    return lax.dot_general(a, b, (((1,), (1,)), ((), ())), preferred_element_type=F32)


def dot_tn(a, b):
    return lax.dot_general(a, b, (((0,), (0,)), ((), ())), preferred_element_type=F32)


def loop(lo, hi, fn):
    def step(i, carry):
        fn(i)
        return carry

    lax.fori_loop(lo, hi, step, 0)


def kernel(
    n_sp, n_tp, cap,
    qw_h, qn_h, lat_h, rk_h, lnw, bk_h, bv_h, sk_h, sv_h, ow_h, on_h, res_h, gain, meta,
    base_t, local_t, gate_h, up_h, down_h,
    out_ref,
    qw, qn, lat, rk, lift, wout, res, gu, down,
    own_lat, lat_all, kbuf, vbuf, att, part, part_in, xs, cs, rx, comb, nx, hid, pd, d1, e1, d2, fin, ret,
    ld_sem, snd, rcv_a, rcv_b, snd_b, rcv_k, snd_k, rcv_c, snd_d, rcv_d1, rcv_d2, rcv_g,
):
    me = lax.axis_index("sp")
    j = lax.axis_index("tp")
    j2 = lax.rem(j + 2, 4)
    j1 = j + 1 - 2 * lax.rem(j, 2)
    j3 = lax.rem(j1 + 2, 4)
    rel = (j, j1, j2, j3)
    tok = lat.shape[0]
    rank = lat.shape[1]
    quarter = res.shape[1]
    experts = gu.shape[0]
    ff = gu.shape[2] // 2
    slots = n_sp * cap
    kw = bk_h.shape[1]
    kn = sk_h.shape[1]
    heads_w = kw // PLAIN_WIDE
    heads_n = kn // PLAIN_SLIM
    piece = tok // n_tp

    barrier = pltpu.get_barrier_semaphore()

    def greet(i):
        pl.semaphore_signal(barrier, inc=1, device_id=(lax.rem(me + i, n_sp), j), device_id_type=MESH)

    loop(1, n_sp, greet)
    for r in (1, 2, 3):
        pl.semaphore_signal(barrier, inc=1, device_id=(me, rel[r]), device_id_type=MESH)

    loads = []

    def load(src, dst):
        c = pltpu.make_async_copy(src, dst, ld_sem.at[len(loads)])
        c.start()
        loads.append(c)
        return c

    first = [load(lat_h, lat), load(rk_h, rk)]
    queries = [load(qw_h, qw), load(qn_h, qn)]
    lifts = [
        load(bk_h, lift.at[:, pl.ds(0, kw)]),
        load(bv_h, lift.at[:, pl.ds(kw, kw)]),
        load(sk_h, lift.at[:, pl.ds(2 * kw, kn)]),
        load(sv_h, lift.at[:, pl.ds(2 * kw + kn, kn)]),
    ]
    outs = [
        load(ow_h, wout.at[pl.ds(0, kw)]),
        load(on_h, wout.at[pl.ds(kw, kn)]),
        load(res_h.at[:, pl.ds(pl.multiple_of(j * quarter, quarter), quarter)], res),
    ]
    weights = [
        load(gate_h.at[0], gu.at[:, :, pl.ds(0, ff)]),
        load(up_h.at[0], gu.at[:, :, pl.ds(ff, ff)]),
    ]
    for e in range(experts):
        weights.append(load(down_h.at[0, e], down.at[pl.ds(e * ff, ff)]))

    lane = lax.broadcasted_iota(jnp.int32, (tok, LANES), 1)
    low = lane < 64
    cb = base_t[0, pl.ds(me, 1), :]
    sb = base_t[1, pl.ds(me, 1), :]
    cl = local_t[0]
    sl = local_t[1]
    cos = cb * cl - sb * sl
    sin = sb * cl + cb * sl
    first_half = lax.rem(lane, 64) < 32
    sin = jnp.where(first_half, -sin, sin)
    ones = jnp.ones_like(cos)
    zeros = jnp.zeros_like(cos)

    def turn(x, c, s):
        swapped = jnp.where(first_half, pltpu.roll(x, 96, 1), pltpu.roll(x, 32, 1))
        return x * c + swapped * s

    for c in first:
        c.wait()
    dup = (lax.broadcasted_iota(jnp.int32, (ROPE, LANES), 0)
           == lax.rem(lax.broadcasted_iota(jnp.int32, (ROPE, LANES), 1), 64)).astype(BF16)
    rk2 = turn(dot(rk[...], dup), cos, sin).astype(BF16)
    x = lat[...].astype(F32)
    rows = (x * lax.rsqrt(jnp.mean(x * x, axis=-1, keepdims=True) + EPSILON) * lnw[...]).astype(BF16)
    own_lat[:, :, 0:rank] = rows.reshape(n_tp, piece, rank)
    own_lat[:, :, rank:] = rk2.reshape(n_tp, piece, LANES)
    lat_all[pl.ds(me, 1), :, :, 0:rank] = rows.reshape(1, n_tp, piece, rank)
    lat_all[pl.ds(me, 1), :, :, rank:] = rk2.reshape(1, n_tp, piece, LANES)

    pl.semaphore_wait(barrier, n_sp - 1 + 3)

    def copy(src, dst, s_sem, r_sem, dev):
        return pltpu.make_async_remote_copy(
            src_ref=src, dst_ref=dst, send_sem=s_sem, recv_sem=r_sem, device_id=dev, device_id_type=MESH
        )

    def lat_sp(dest):
        return copy(own_lat.at[j], lat_all.at[me, j], snd.at[dest, 0], rcv_a.at[me, 0], (dest, j))

    loop(me + 1, n_sp, lambda d: lat_sp(d).start())

    meta_v = meta[...]
    route = meta_v[0:1, :]
    gcol = lax.broadcasted_iota(jnp.int32, (max(n_sp, 8), tok), 0).astype(F32)
    member = (gcol == route).astype(F32)
    upper = (lax.broadcasted_iota(jnp.int32, (tok, tok), 0)
             <= lax.broadcasted_iota(jnp.int32, (tok, tok), 1)).astype(BF16)
    ranks = dot(member.astype(BF16), upper)
    rank_row = jnp.sum(member * ranks, axis=0, keepdims=True) - 1.0
    slot_row = route * float(cap) + rank_row
    slot_iota = lax.broadcasted_iota(jnp.int32, (slots, tok), 0).astype(F32)
    place = (slot_iota == slot_row).astype(BF16)
    eiota = lax.broadcasted_iota(jnp.int32, (LANES, tok), 0).astype(F32)
    total = meta_v[4:5, :] + meta_v[5:6, :]
    combine = jnp.zeros((LANES, tok), F32)
    for k in range(2):
        share = meta_v[3:4, :] * meta_v[4 + k:5 + k, :] / total
        combine = combine + jnp.where(eiota == meta_v[1 + k:2 + k, :], share, 0.0)
    cs_v = dot_nt(place, combine.astype(BF16)).astype(BF16).reshape(n_sp, cap, LANES)
    cs[...] = cs_v

    for c in queries:
        c.wait()

    def tile(ref, k):
        return ref[:, k * LANES:(k + 1) * LANES].astype(F32)

    cos_a, sin_a = jnp.where(low, cos, ones), jnp.where(low, sin, zeros)
    cos_b, sin_b = jnp.where(low, ones, cos), jnp.where(low, zeros, sin)
    q_wide = []
    for h in range(heads_w):
        start = h * (PLAIN_WIDE + ROPE)
        if start % LANES == 0:
            k = start // LANES
            nope = tile(qw, k)
            rot = turn(tile(qw, k + 1), cos_a, sin_a)
        else:
            k = start // LANES
            t1 = pltpu.roll(tile(qw, k), 64, 1)
            t2 = pltpu.roll(tile(qw, k + 1), 64, 1)
            nope = jnp.where(low, t1, t2)
            rot = turn(t2, cos_a, sin_a)
        q_wide.append(jnp.concatenate(
            [nope.astype(BF16), jnp.where(low, rot, zeros).astype(BF16)], axis=1))
    q_slim = []
    for h in range(heads_n):
        y = turn(tile(qn, h), cos_b, sin_b)
        if h % 2 == 1:
            y = pltpu.roll(y, 64, 1)
        q_slim.append(y.astype(BF16))

    kbuf[...] = jnp.zeros_like(kbuf)
    vbuf[...] = jnp.zeros_like(vbuf)

    def comb_sp(dest):
        return copy(cs.at[dest], comb.at[me], snd_k.at[dest], rcv_k.at[me], (dest, j))

    def others(fn):
        loop(1, n_sp, lambda i: fn(lax.rem(me + i, n_sp)))

    others(lambda d: comb_sp(d).start())
    comb[pl.ds(me, 1)] = dot_nt(
        (lax.broadcasted_iota(jnp.int32, (cap, tok), 0).astype(F32) + (me * cap).astype(F32)
         == slot_row).astype(BF16), combine.astype(BF16)).astype(BF16)[None]

    def gather(buf, s, r, rcv):
        if r == 2:
            return copy(buf.at[s, j], buf.at[s, j], snd.at[s, 1], rcv.at[s, 2], (me, j2))
        if r == 1:
            return copy(buf.at[s, j], buf.at[s, j], snd.at[s, 2], rcv.at[s, 1], (me, j1))
        return copy(buf.at[s, j2], buf.at[s, j2], snd.at[s, 3], rcv.at[s, 3], (me, j1))

    def arrived(buf, s, r, rcv):
        copy(buf.at[s, rel[r]], buf.at[s, rel[r]], snd.at[s, 0], rcv.at[s, r], (me, j1)).wait_recv()

    for c in lifts:
        c.wait()

    def expand(s):
        rows_s = lat_all[pl.ds(s, 1)].reshape(tok, rank + LANES)
        kv = dot(rows_s[:, 0:rank], lift[...]).astype(BF16)
        rot = rows_s[:, rank:]
        at = pl.ds(pl.multiple_of(s * tok, tok), tok)
        for h in range(heads_w):
            kbuf[at, h * 256:h * 256 + 128] = kv[:, h * 128:(h + 1) * 128]
            kbuf[at, h * 256 + 128:(h + 1) * 256] = rot
        vbuf[at, 0:kw] = kv[:, kw:2 * kw]
        off = heads_w * 256
        for h in range(heads_n):
            pair = kv[:, 2 * kw + (h // 2) * 128:2 * kw + (h // 2 + 1) * 128]
            mixed = jnp.where(low, pair, rot) if h % 2 == 0 else jnp.where(low, rot, pair)
            kbuf[at, off + h * 128:off + (h + 1) * 128] = mixed
        vbuf[at, kw:] = kv[:, 2 * kw + kn:]

    def a1(i):
        s = me - 1 - i
        arrived(lat_all, s, 0, rcv_a)
        gather(lat_all, s, 2, rcv_a).start()
        gather(lat_all, s, 1, rcv_a).start()

    def a2(i):
        s = me - 1 - i
        arrived(lat_all, s, 2, rcv_a)
        gather(lat_all, s, 3, rcv_a).start()

    def a3(i):
        s = me - 1 - i
        arrived(lat_all, s, 1, rcv_a)
        arrived(lat_all, s, 3, rcv_a)
        expand(s)

    expand(me)
    loop(0, me, a1)
    loop(0, me, a2)
    loop(0, me, a3)

    keys = n_sp * tok
    chunk = min(keys, 1024)
    n_chunk = keys // chunk

    def head(q, kcol, kwid, vcol, scale):
        def scores(c):
            at = pl.ds(pl.multiple_of(c * chunk, chunk), chunk)
            sc = dot_nt(q, kbuf[at, kcol:kcol + kwid]) * scale
            kpos = c * chunk + lax.broadcasted_iota(jnp.int32, (tok, chunk), 1)
            qpos = me * tok + lax.broadcasted_iota(jnp.int32, (tok, chunk), 0)
            return jnp.where(kpos <= qpos, sc, MASKED), vbuf[at, vcol:vcol + LANES]

        if n_chunk == 1:
            sc, v = scores(0)
            p = jnp.exp(sc - jnp.max(sc, axis=-1, keepdims=True))
            return dot(p.astype(BF16), v) / jnp.sum(p, axis=-1, keepdims=True)

        def step(c, carry):
            m, l, acc = carry
            sc, v = scores(c)
            m2 = jnp.maximum(m, jnp.max(sc, axis=-1, keepdims=True))
            keep = jnp.exp(m - m2)
            p = jnp.exp(sc - m2)
            return m2, l * keep + jnp.sum(p, axis=-1, keepdims=True), acc * keep + dot(p.astype(BF16), v)

        init = (jnp.full((tok, 1), MASKED, F32), jnp.zeros((tok, 1), F32), jnp.zeros((tok, LANES), F32))
        m, l, acc = lax.fori_loop(0, n_chunk, step, init)
        return acc / l

    for h in range(heads_w):
        o = head(q_wide[h], h * 256, 256, h * 128, (PLAIN_WIDE + ROPE) ** -0.5)
        att[:, h * 128:(h + 1) * 128] = o.astype(BF16)
    off = heads_w * 256
    for h in range(0, heads_n, 2):
        o0 = head(q_slim[h], off + h * 128, 128, kw + (h // 2) * 128, (PLAIN_SLIM + ROPE) ** -0.5)
        o1 = head(q_slim[h + 1], off + (h + 1) * 128, 128, kw + (h // 2) * 128, (PLAIN_SLIM + ROPE) ** -0.5)
        att[:, kw + (h // 2) * 128:kw + (h // 2 + 1) * 128] = jnp.where(low, o0, o1).astype(BF16)

    for c in outs:
        c.wait()

    def swap_b(r):
        return copy(part.at[r], part_in.at[r - 1], snd_b.at[r - 1], rcv_b.at[r - 1], (me, rel[r]))

    for r in (2, 3, 1, 0):
        cols = pl.ds(pl.multiple_of(rel[r] * quarter, quarter), quarter)
        y = dot(att[...], wout[:, cols])
        if r == 0:
            mine = y.astype(BF16).astype(F32)
        else:
            part[r] = y.astype(BF16)
            swap_b(r).start()

    loop(me + 1, n_sp, lambda d: lat_sp(d).wait_send())

    def a_done(s):
        for r in (1, 2, 3):
            gather(lat_all, s, r, rcv_a).wait_send()

    loop(0, me, a_done)

    for r in (1, 2, 3):
        swap_b(r).wait_recv()
        mine = mine + part_in[r - 1].astype(F32)
    stream = (res[...].astype(F32) + mine).astype(BF16)

    xs[...] = dot(place, stream).astype(BF16).reshape(n_sp, cap, quarter)
    own_rows = (lax.broadcasted_iota(jnp.int32, (cap, tok), 0).astype(F32) + (me * cap).astype(F32)
                == slot_row).astype(BF16)
    rx[pl.ds(me, 1), pl.ds(j, 1)] = dot(own_rows, stream).astype(BF16)[None, None]

    def rows_sp(dest):
        return copy(xs.at[dest], rx.at[me, j], snd.at[dest, 0], rcv_c.at[me, 0], (dest, j))

    others(lambda d: rows_sp(d).start())

    def c1(s):
        gather(rx, s, 2, rcv_c).start()
        gather(rx, s, 1, rcv_c).start()

    c1(me)

    def c1w(s):
        arrived(rx, s, 0, rcv_c)
        c1(s)

    def c2(s):
        arrived(rx, s, 2, rcv_c)
        gather(rx, s, 3, rcv_c).start()

    def c3(s):
        arrived(rx, s, 1, rcv_c)
        arrived(rx, s, 3, rcv_c)

    others(c1w)
    c2(me)
    others(c2)
    for c in weights:
        c.wait()
    others(lambda s: copy(cs.at[s], comb.at[s], snd_k.at[s], rcv_k.at[s], (s, j)).wait_recv())
    c3(me)
    others(c3)

    blk = min(slots, 256)
    per = blk // cap
    for b in range(slots // blk):
        sq = jnp.zeros((blk, 1), F32)
        for q in range(n_tp):
            v = rx[b * per:(b + 1) * per, q].reshape(blk, quarter).astype(F32)
            sq = sq + jnp.sum(v * v, axis=-1, keepdims=True)
        inv = lax.rsqrt(sq / (n_tp * quarter) + EPSILON)
        for q in range(n_tp):
            v = rx[b * per:(b + 1) * per, q].reshape(blk, quarter).astype(F32)
            nx[:, q * quarter:(q + 1) * quarter] = (v * inv * gain[:, q * quarter:(q + 1) * quarter]).astype(BF16)
        w = comb[b * per:(b + 1) * per].reshape(blk, LANES).astype(F32)
        for e in range(experts):
            y = dot(nx[...], gu[e])
            g, u = y[:, 0:ff], y[:, ff:]
            hid[b * blk:(b + 1) * blk, e * ff:(e + 1) * ff] = (
                g / (1.0 + jnp.exp(-g)) * u * w[:, e:e + 1]).astype(BF16)

    def swap_d(i):
        return copy(pd.at[3 if i else 1], d1.at[i], snd_d.at[i], rcv_d1.at[i], (me, j1))

    for r in (3, 1, 2, 0):
        cols = pl.ds(pl.multiple_of(rel[r] * quarter, quarter), quarter)
        for b in range(slots // blk):
            y = dot(hid[b * blk:(b + 1) * blk], down[:, cols]).astype(BF16)
            pd[r, b * per:(b + 1) * per] = y.reshape(per, cap, quarter)
        if r == 3:
            swap_d(1).start()
        if r == 1:
            swap_d(0).start()

    others(lambda d: rows_sp(d).wait_send())

    def c_done(s):
        for r in (1, 2, 3):
            gather(rx, s, r, rcv_c).wait_send()

    c_done(me)
    others(c_done)
    others(lambda d: comb_sp(d).wait_send())

    def pair_d(s):
        return copy(e1.at[s], d2.at[s], snd.at[s, 0], rcv_d2.at[s], (me, j2))

    def home(s):
        return copy(fin.at[s], ret.at[me], snd.at[s, 1], rcv_g.at[me], (s, j))

    swap_d(1).wait_recv()

    def d_pair(s):
        at = pl.ds(s, 1)
        e1[at] = (pd[2, at].astype(F32) + d1[1, at].astype(F32)).astype(BF16)
        pair_d(s).start()

    others(d_pair)
    d_pair(me)
    swap_d(0).wait_recv()

    def summed(s):
        at = pl.ds(s, 1)
        pair_d(s).wait_recv()
        return (pd[0, at].astype(F32) + d1[0, at].astype(F32) + d2[at].astype(F32)).astype(BF16)

    def d_home(s):
        fin[pl.ds(s, 1)] = summed(s)
        home(s).start()

    others(d_home)
    ret[pl.ds(me, 1)] = summed(me)
    others(lambda s: copy(fin.at[s], ret.at[s], snd.at[s, 1], rcv_g.at[s], (s, j)).wait_recv())
    moe = dot_tn(place, ret[...].reshape(slots, quarter))
    out_ref[...] = (stream.astype(F32) + moe).astype(BF16)

    for r in (1, 2, 3):
        swap_b(r).wait_send()
    swap_d(0).wait_send()
    swap_d(1).wait_send()
    pair_d(me).wait_send()

    def tail(s):
        pair_d(s).wait_send()
        home(s).wait_send()

    others(tail)


def body(
    n_sp, n_tp,
    query_wide, query_narrow, latent, rope_key, latent_norm_weight, broad_key_lift, broad_value_lift,
    slim_key_lift, slim_value_lift, out_wide, out_narrow, resid, ffn_gain, group_route, expert_pair,
    group_prob, expert_prob, gate_weight, up_weight, down_weight,
):
    tok, rank = latent.shape
    width = resid.shape[1]
    quarter = width // n_tp
    experts, _, ff = gate_weight.shape[1:]
    cap = max(2 * tok // n_sp, 16)
    kw, kn = broad_key_lift.shape[1], slim_key_lift.shape[1]
    heads_w, heads_n = kw // PLAIN_WIDE, kn // PLAIN_SLIM
    keys = n_sp * tok
    slots = n_sp * cap
    blk = min(slots, 256)

    freq = (1.0 / ROPE_BASE ** (np.arange(0, ROPE, 2).astype(np.float32) / np.float32(ROPE))).astype(np.float32)
    freq = np.tile(freq.astype(np.float64), LANES // (ROPE // 2))[None, :]
    base = (np.arange(n_sp) * tok)[:, None] * freq
    local = np.arange(tok)[:, None] * freq
    base_t = jnp.asarray(np.stack([np.cos(base), np.sin(base)]).astype(np.float32))
    local_t = jnp.asarray(np.stack([np.cos(local), np.sin(local)]).astype(np.float32))
    pair = expert_pair.astype(F32)
    meta = jnp.stack([
        group_route.astype(F32), pair[:, 0], pair[:, 1], group_prob, expert_prob[:, 0], expert_prob[:, 1],
        group_prob, group_prob,
    ])
    vm = pl.BlockSpec(memory_space=pltpu.VMEM)
    hb = pl.BlockSpec(memory_space=pl.ANY)
    dma = pltpu.SemaphoreType.DMA
    scratch = [
        pltpu.VMEM(query_wide.shape, BF16), pltpu.VMEM(query_narrow.shape, BF16),
        pltpu.VMEM(latent.shape, BF16), pltpu.VMEM(rope_key.shape, BF16),
        pltpu.VMEM((rank, 2 * kw + 2 * kn), BF16),
        pltpu.VMEM((kw + kn, width), BF16),
        pltpu.VMEM((tok, quarter), BF16),
        pltpu.VMEM((experts, width, 2 * ff), BF16),
        pltpu.VMEM((experts * ff, width), BF16),
        pltpu.VMEM((n_tp, tok // n_tp, rank + LANES), BF16),
        pltpu.VMEM((n_sp, n_tp, tok // n_tp, rank + LANES), BF16),
        pltpu.VMEM((keys, heads_w * 256 + heads_n * 128), BF16),
        pltpu.VMEM((keys, kw + kn), BF16),
        pltpu.VMEM((tok, kw + kn), BF16),
        pltpu.VMEM((4, tok, quarter), BF16),
        pltpu.VMEM((3, tok, quarter), BF16),
        pltpu.VMEM((n_sp, cap, quarter), BF16),
        pltpu.VMEM((n_sp, cap, LANES), BF16),
        pltpu.VMEM((n_sp, n_tp, cap, quarter), BF16),
        pltpu.VMEM((n_sp, cap, LANES), BF16),
        pltpu.VMEM((blk, width), BF16),
        pltpu.VMEM((slots, experts * ff), BF16),
        pltpu.VMEM((4, n_sp, cap, quarter), BF16),
        pltpu.VMEM((2, n_sp, cap, quarter), BF16),
        pltpu.VMEM((n_sp, cap, quarter), BF16),
        pltpu.VMEM((n_sp, cap, quarter), BF16),
        pltpu.VMEM((n_sp, cap, quarter), BF16),
        pltpu.VMEM((n_sp, cap, quarter), BF16),
        dma((13 + experts,)), dma((n_sp, 4)), dma((n_sp, 4)), dma((3,)), dma((3,)), dma((n_sp,)), dma((n_sp,)),
        dma((n_sp, 4)), dma((2,)), dma((2,)), dma((n_sp,)), dma((n_sp,)),
    ]
    call = pl.pallas_call(
        functools.partial(kernel, n_sp, n_tp, cap),
        out_shape=jax.ShapeDtypeStruct((tok, quarter), BF16),
        in_specs=[hb, hb, hb, hb, vm, hb, hb, hb, hb, hb, hb, hb, vm, vm, vm, vm, hb, hb, hb],
        out_specs=vm,
        scratch_shapes=scratch,
        compiler_params=pltpu.CompilerParams(
            collective_id=0, has_side_effects=True, vmem_limit_bytes=67043328
        ),
    )
    return call(
        query_wide, query_narrow, latent, rope_key, latent_norm_weight[None, :], broad_key_lift,
        broad_value_lift, slim_key_lift, slim_value_lift, out_wide, out_narrow, resid, ffn_gain[None, :], meta,
        base_t, local_t, gate_weight, up_weight, down_weight,
    )


def solution(mesh):
    sizes = dict(mesh.shape)
    placed = (
        P("sp", "tp"), P("sp", "tp"), P("sp", None), P("sp", None), P(), P(None, "tp"), P(None, "tp"),
        P(None, "tp"), P(None, "tp"), P("tp", None), P("tp", None), P("sp", None), P(), P("sp"),
        P("sp", None), P("sp"), P("sp", None), P("sp", None, None, "tp"), P("sp", None, None, "tp"),
        P("sp", None, "tp", None),
    )
    return jax.shard_map(
        functools.partial(body, sizes["sp"], sizes["tp"]),
        mesh=mesh, in_specs=placed, out_specs=P("sp", "tp"), check_vma=False,
    )
```

```python
import functools

import jax
import jax.numpy as jnp
import numpy as np
from jax import lax
from jax.experimental import pallas as pl
from jax.experimental.pallas import tpu as pltpu
from jax.sharding import PartitionSpec as P

PLAIN_WIDE = 128
PLAIN_SLIM = 64
ROPE = 64
LANES = 128
ROPE_BASE = 10000.0
EPSILON = 1e-06
MASKED = -1e30
F32 = jnp.float32
BF16 = jnp.bfloat16
MESH = pl.DeviceIdType.MESH


def dot(a, b):
    return jnp.dot(a, b, preferred_element_type=F32)


def dot_nt(a, b):
    return lax.dot_general(a, b, (((1,), (1,)), ((), ())), preferred_element_type=F32)


def dot_tn(a, b):
    return lax.dot_general(a, b, (((0,), (0,)), ((), ())), preferred_element_type=F32)


def loop(lo, hi, fn):
    def step(i, carry):
        fn(i)
        return carry

    lax.fori_loop(lo, hi, step, 0)


def kernel(
    n_sp, n_tp, cap,
    qw_h, qn_h, lat_h, rk_h, lnw, bk_h, bv_h, sk_h, sv_h, ow_h, on_h, res_h, gain, route_r, pair_r, gprob_r, eprob_r,
    base_t, local_t, gate_h, up_h, down_h,
    out_ref,
    qw, qn, lat, rk, lift, wout, res, gu, down,
    own_lat, lat_all, kbuf, vbuf, att, part, part_in, xs, cs, rx, comb, nx, hid, pd, d1, e1, d2, fin, ret,
    ld_sem, snd, rcv_a, rcv_b, snd_b, rcv_k, snd_k, rcv_c, snd_d, rcv_d1, rcv_d2, rcv_g,
):
    me = lax.axis_index("sp")
    j = lax.axis_index("tp")
    j2 = lax.rem(j + 2, 4)
    j1 = j + 1 - 2 * lax.rem(j, 2)
    j3 = lax.rem(j1 + 2, 4)
    rel = (j, j1, j2, j3)
    tok = lat.shape[0]
    rank = lat.shape[1]
    quarter = res.shape[1]
    experts = gu.shape[0]
    ff = gu.shape[2] // 2
    slots = n_sp * cap
    kw = bk_h.shape[1]
    kn = sk_h.shape[1]
    heads_w = kw // PLAIN_WIDE
    heads_n = kn // PLAIN_SLIM
    piece = tok // n_tp

    barrier = pltpu.get_barrier_semaphore()

    def greet(i):
        pl.semaphore_signal(barrier, inc=1, device_id=(lax.rem(me + i, n_sp), j), device_id_type=MESH)

    loop(1, n_sp, greet)
    for r in (1, 2, 3):
        pl.semaphore_signal(barrier, inc=1, device_id=(me, rel[r]), device_id_type=MESH)

    loads = []

    def load(src, dst):
        c = pltpu.make_async_copy(src, dst, ld_sem.at[len(loads)])
        c.start()
        loads.append(c)
        return c

    first = [load(lat_h, lat), load(rk_h, rk)]
    queries = [load(qw_h, qw), load(qn_h, qn)]
    lifts = [
        load(bk_h, lift.at[:, pl.ds(0, kw)]),
        load(bv_h, lift.at[:, pl.ds(kw, kw)]),
        load(sk_h, lift.at[:, pl.ds(2 * kw, kn)]),
        load(sv_h, lift.at[:, pl.ds(2 * kw + kn, kn)]),
    ]
    outs = [
        load(ow_h, wout.at[pl.ds(0, kw)]),
        load(on_h, wout.at[pl.ds(kw, kn)]),
        load(res_h.at[:, pl.ds(pl.multiple_of(j * quarter, quarter), quarter)], res),
    ]
    weights = [
        load(gate_h.at[0], gu.at[:, :, pl.ds(0, ff)]),
        load(up_h.at[0], gu.at[:, :, pl.ds(ff, ff)]),
    ]
    for e in range(experts):
        weights.append(load(down_h.at[0, e], down.at[pl.ds(e * ff, ff)]))

    lane = lax.broadcasted_iota(jnp.int32, (tok, LANES), 1)
    low = lane < 64
    cb = base_t[0, pl.ds(me, 1), :]
    sb = base_t[1, pl.ds(me, 1), :]
    cl = local_t[0]
    sl = local_t[1]
    cos = cb * cl - sb * sl
    sin = sb * cl + cb * sl
    first_half = lax.rem(lane, 64) < 32
    sin = jnp.where(first_half, -sin, sin)
    ones = jnp.ones_like(cos)
    zeros = jnp.zeros_like(cos)

    def turn(x, c, s):
        swapped = jnp.where(first_half, pltpu.roll(x, 96, 1), pltpu.roll(x, 32, 1))
        return x * c + swapped * s

    for c in first:
        c.wait()
    dup = (lax.broadcasted_iota(jnp.int32, (ROPE, LANES), 0)
           == lax.rem(lax.broadcasted_iota(jnp.int32, (ROPE, LANES), 1), 64)).astype(BF16)
    rk2 = turn(dot_tn(rk[...], dup), cos, sin).astype(BF16)
    x = lat[...].astype(F32)
    rows = (x * lax.rsqrt(jnp.mean(x * x, axis=-1, keepdims=True) + EPSILON) * lnw[...]).astype(BF16)
    own_lat[:, :, 0:rank] = rows.reshape(n_tp, piece, rank)
    own_lat[:, :, rank:] = rk2.reshape(n_tp, piece, LANES)
    lat_all[pl.ds(me, 1), :, :, 0:rank] = rows.reshape(1, n_tp, piece, rank)
    lat_all[pl.ds(me, 1), :, :, rank:] = rk2.reshape(1, n_tp, piece, LANES)

    pl.semaphore_wait(barrier, n_sp - 1 + 3)

    def copy(src, dst, s_sem, r_sem, dev):
        return pltpu.make_async_remote_copy(
            src_ref=src, dst_ref=dst, send_sem=s_sem, recv_sem=r_sem, device_id=dev, device_id_type=MESH
        )

    odd = lax.rem(me, 2)
    other = me + 1 - 2 * odd

    def lat_sp(dest):
        return copy(own_lat.at[j], lat_all.at[me, j], snd.at[dest, 0], rcv_a.at[me, 0], (dest, j))

    def lat_pass(s):
        return copy(lat_all.at[s, j], lat_all.at[s, j], snd.at[s, 0], rcv_a.at[s, 0], (other, j))

    later = lax.div(n_sp - 1 - me, 2)

    @pl.when(odd == 0)
    def _():
        lat_sp(other).start()

    loop(0, later, lambda i: lat_sp(me + 2 + 2 * i).start())

    route = route_r[...].astype(F32)
    gcol = lax.broadcasted_iota(jnp.int32, (max(n_sp, 8), tok), 0).astype(F32)
    member = (gcol == route).astype(F32)
    upper = (lax.broadcasted_iota(jnp.int32, (tok, tok), 0)
             <= lax.broadcasted_iota(jnp.int32, (tok, tok), 1)).astype(BF16)
    ranks = dot(member.astype(BF16), upper)
    rank_row = jnp.sum(member * ranks, axis=0, keepdims=True) - 1.0
    slot_row = route * float(cap) + rank_row
    slot_iota = lax.broadcasted_iota(jnp.int32, (slots, tok), 0).astype(F32)
    place = (slot_iota == slot_row).astype(BF16)
    eiota = lax.broadcasted_iota(jnp.int32, (LANES, tok), 0).astype(F32)
    pair = pair_r[...].astype(F32)
    total = eprob_r[0:1, :] + eprob_r[1:2, :]
    combine = jnp.zeros((LANES, tok), F32)
    for k in range(2):
        share = gprob_r[...] * eprob_r[k:k + 1, :] / total
        combine = combine + jnp.where(eiota == pair[k:k + 1, :], share, 0.0)
    cs_v = dot_nt(place, combine.astype(BF16)).astype(BF16).reshape(n_sp, cap, LANES)
    cs[...] = cs_v

    for c in queries:
        c.wait()

    def tile(ref, k):
        return ref[:, k * LANES:(k + 1) * LANES].astype(F32)

    cos_a, sin_a = jnp.where(low, cos, ones), jnp.where(low, sin, zeros)
    cos_b, sin_b = jnp.where(low, ones, cos), jnp.where(low, zeros, sin)
    q_wide = []
    for h in range(heads_w):
        start = h * (PLAIN_WIDE + ROPE)
        if start % LANES == 0:
            k = start // LANES
            nope = tile(qw, k)
            rot = turn(tile(qw, k + 1), cos_a, sin_a)
        else:
            k = start // LANES
            t1 = pltpu.roll(tile(qw, k), 64, 1)
            t2 = pltpu.roll(tile(qw, k + 1), 64, 1)
            nope = jnp.where(low, t1, t2)
            rot = turn(t2, cos_a, sin_a)
        q_wide.append(jnp.concatenate(
            [nope.astype(BF16), jnp.where(low, rot, zeros).astype(BF16)], axis=1))
    q_slim = []
    for h in range(heads_n):
        y = turn(tile(qn, h), cos_b, sin_b)
        if h % 2 == 1:
            y = pltpu.roll(y, 64, 1)
        q_slim.append(y.astype(BF16))

    kbuf[...] = jnp.zeros_like(kbuf)
    vbuf[...] = jnp.zeros_like(vbuf)

    def comb_sp(dest):
        return copy(cs.at[dest], comb.at[me], snd_k.at[dest], rcv_k.at[me], (dest, j))

    def others(fn):
        loop(1, n_sp, lambda i: fn(lax.rem(me + i, n_sp)))

    others(lambda d: comb_sp(d).start())
    comb[pl.ds(me, 1)] = dot_nt(
        (lax.broadcasted_iota(jnp.int32, (cap, tok), 0).astype(F32) + (me * cap).astype(F32)
         == slot_row).astype(BF16), combine.astype(BF16)).astype(BF16)[None]

    def gather(buf, s, r, rcv):
        if r == 2:
            return copy(buf.at[s, j], buf.at[s, j], snd.at[s, 1], rcv.at[s, 2], (me, j2))
        if r == 1:
            return copy(buf.at[s, j], buf.at[s, j], snd.at[s, 2], rcv.at[s, 1], (me, j1))
        return copy(buf.at[s, j2], buf.at[s, j2], snd.at[s, 3], rcv.at[s, 3], (me, j1))

    def arrived(buf, s, r, rcv):
        copy(buf.at[s, rel[r]], buf.at[s, rel[r]], snd.at[s, 0], rcv.at[s, r], (me, j1)).wait_recv()

    for c in lifts:
        c.wait()

    def expand(s):
        rows_s = lat_all[pl.ds(s, 1)].reshape(tok, rank + LANES)
        kv = dot(rows_s[:, 0:rank], lift[...]).astype(BF16)
        rot = rows_s[:, rank:]
        at = pl.ds(pl.multiple_of(s * tok, tok), tok)
        for h in range(heads_w):
            kbuf[at, h * 256:h * 256 + 128] = kv[:, h * 128:(h + 1) * 128]
            kbuf[at, h * 256 + 128:(h + 1) * 256] = rot
        vbuf[at, 0:kw] = kv[:, kw:2 * kw]
        off = heads_w * 256
        for h in range(heads_n):
            pair = kv[:, 2 * kw + (h // 2) * 128:2 * kw + (h // 2 + 1) * 128]
            mixed = jnp.where(low, pair, rot) if h % 2 == 0 else jnp.where(low, rot, pair)
            kbuf[at, off + h * 128:off + (h + 1) * 128] = mixed
        vbuf[at, kw:] = kv[:, 2 * kw + kn:]

    def a1(i, s):
        arrived(lat_all, s, 0, rcv_a)
        gather(lat_all, s, 2, rcv_a).start()
        gather(lat_all, s, 1, rcv_a).start()

        @pl.when(lax.rem(i, 2) == 0)
        def _():
            lat_pass(s).start()

    def a2(i, s):
        arrived(lat_all, s, 2, rcv_a)
        gather(lat_all, s, 3, rcv_a).start()

    def a3(i, s):
        arrived(lat_all, s, 1, rcv_a)
        arrived(lat_all, s, 3, rcv_a)
        expand(s)

    steps = me + odd

    def a_step(t):
        for lag, fn in ((0, a1), (2, a2), (3, a3)):
            i = t - lag
            i0 = jnp.maximum(i, 0)
            s = me - 2 - i0 + 2 * lax.rem(i0, 2)

            @pl.when((i >= 0) & (i < steps) & (s >= 0))
            def _():
                fn(i0, s)

    expand(me)
    loop(0, steps + 3, a_step)

    keys = n_sp * tok
    chunk = min(keys, 1024)
    n_chunk = keys // chunk

    def head(q, kcol, kwid, vcol, scale):
        def scores(c):
            at = pl.ds(pl.multiple_of(c * chunk, chunk), chunk)
            sc = dot_nt(q, kbuf[at, kcol:kcol + kwid]) * scale
            kpos = c * chunk + lax.broadcasted_iota(jnp.int32, (tok, chunk), 1)
            qpos = me * tok + lax.broadcasted_iota(jnp.int32, (tok, chunk), 0)
            return jnp.where(kpos <= qpos, sc, MASKED), vbuf[at, vcol:vcol + LANES]

        if n_chunk == 1:
            sc, v = scores(0)
            p = jnp.exp(sc - jnp.max(sc, axis=-1, keepdims=True))
            return dot(p.astype(BF16), v) / jnp.sum(p, axis=-1, keepdims=True)

        def step(c, carry):
            m, l, acc = carry
            sc, v = scores(c)
            m2 = jnp.maximum(m, jnp.max(sc, axis=-1, keepdims=True))
            keep = jnp.exp(m - m2)
            p = jnp.exp(sc - m2)
            return m2, l * keep + jnp.sum(p, axis=-1, keepdims=True), acc * keep + dot(p.astype(BF16), v)

        init = (jnp.full((tok, 1), MASKED, F32), jnp.zeros((tok, 1), F32), jnp.zeros((tok, LANES), F32))
        m, l, acc = lax.fori_loop(0, n_chunk, step, init)
        return acc / l

    for h in range(heads_w):
        o = head(q_wide[h], h * 256, 256, h * 128, (PLAIN_WIDE + ROPE) ** -0.5)
        att[:, h * 128:(h + 1) * 128] = o.astype(BF16)
    off = heads_w * 256
    for h in range(0, heads_n, 2):
        o0 = head(q_slim[h], off + h * 128, 128, kw + (h // 2) * 128, (PLAIN_SLIM + ROPE) ** -0.5)
        o1 = head(q_slim[h + 1], off + (h + 1) * 128, 128, kw + (h // 2) * 128, (PLAIN_SLIM + ROPE) ** -0.5)
        att[:, kw + (h // 2) * 128:kw + (h // 2 + 1) * 128] = jnp.where(low, o0, o1).astype(BF16)

    for c in outs:
        c.wait()

    def swap_b(r):
        slot, dest = {1: (0, j1), 2: (2, j2), 3: (1, j1)}[r]
        return copy(part.at[r], part_in.at[slot], snd_b.at[slot], rcv_b.at[slot], (me, dest))

    def project(r):
        cols = pl.ds(pl.multiple_of(rel[r] * quarter, quarter), quarter)
        return dot(att[...], wout[:, cols])

    for r in (3, 1):
        part[r] = project(r).astype(BF16)
        swap_b(r).start()
    crossing = project(2)
    swap_b(3).wait_recv()
    part[2] = (crossing + part_in[1].astype(F32)).astype(BF16)
    swap_b(2).start()
    mine = project(0)

    @pl.when(odd == 0)
    def _():
        lat_sp(other).wait_send()

    loop(0, later, lambda i: lat_sp(me + 2 + 2 * i).wait_send())
    loop(0, lax.div(me, 2), lambda i: lat_pass(me - 2 - 2 * i).wait_send())

    def a_done(s):
        for r in (1, 2, 3):
            gather(lat_all, s, r, rcv_a).wait_send()

    loop(0, me, a_done)

    swap_b(1).wait_recv()
    swap_b(2).wait_recv()
    mine = mine + part_in[0].astype(F32) + part_in[2].astype(F32)
    stream = (res[...].astype(F32) + mine).astype(BF16)

    xs[...] = dot(place, stream).astype(BF16).reshape(n_sp, cap, quarter)
    own_rows = (lax.broadcasted_iota(jnp.int32, (cap, tok), 0).astype(F32) + (me * cap).astype(F32)
                == slot_row).astype(BF16)
    rx[pl.ds(me, 1), pl.ds(j, 1)] = dot(own_rows, stream).astype(BF16)[None, None]

    def rows_sp(dest):
        return copy(xs.at[dest], rx.at[me, j], snd.at[dest, 0], rcv_c.at[me, 0], (dest, j))

    others(lambda d: rows_sp(d).start())

    def source(i):
        return lax.rem(me - i + n_sp, n_sp)

    def c1(s):
        gather(rx, s, 2, rcv_c).start()
        gather(rx, s, 1, rcv_c).start()

    def c2(s):
        arrived(rx, s, 2, rcv_c)
        gather(rx, s, 3, rcv_c).start()

    def c3(s):
        arrived(rx, s, 1, rcv_c)
        arrived(rx, s, 3, rcv_c)

    c1(me)

    def c_step(t):
        @pl.when(t < n_sp)
        def _():
            arrived(rx, source(t), 0, rcv_c)
            c1(source(t))

        @pl.when(t >= 2)
        def _():
            c2(source(jnp.maximum(t - 2, 0)))

    loop(1, n_sp + 2, c_step)
    for c in weights:
        c.wait()
    others(lambda s: copy(cs.at[s], comb.at[s], snd_k.at[s], rcv_k.at[s], (s, j)).wait_recv())
    loop(0, n_sp, lambda i: c3(source(i)))

    blk = min(slots, 256)
    per = blk // cap
    for b in range(slots // blk):
        sq = jnp.zeros((blk, 1), F32)
        for q in range(n_tp):
            v = rx[b * per:(b + 1) * per, q].reshape(blk, quarter).astype(F32)
            sq = sq + jnp.sum(v * v, axis=-1, keepdims=True)
        inv = lax.rsqrt(sq / (n_tp * quarter) + EPSILON)
        for q in range(n_tp):
            v = rx[b * per:(b + 1) * per, q].reshape(blk, quarter).astype(F32)
            nx[:, q * quarter:(q + 1) * quarter] = (v * inv * gain[:, q * quarter:(q + 1) * quarter]).astype(BF16)
        w = comb[b * per:(b + 1) * per].reshape(blk, LANES).astype(F32)
        for e in range(experts):
            y = dot(nx[...], gu[e])
            g, u = y[:, 0:ff], y[:, ff:]
            hid[b * blk:(b + 1) * blk, e * ff:(e + 1) * ff] = (
                g / (1.0 + jnp.exp(-g)) * u * w[:, e:e + 1]).astype(BF16)

    def swap_d(i):
        return copy(pd.at[3 if i else 1], d1.at[i], snd_d.at[i], rcv_d1.at[i], (me, j1))

    def product(r):
        cols = pl.ds(pl.multiple_of(rel[r] * quarter, quarter), quarter)
        for b in range(slots // blk):
            y = dot(hid[b * blk:(b + 1) * blk], down[:, cols]).astype(BF16)
            pd[r, b * per:(b + 1) * per] = y.reshape(per, cap, quarter)

    product(3)
    swap_d(1).start()
    product(1)
    swap_d(0).start()
    product(2)

    others(lambda d: rows_sp(d).wait_send())

    def c_done(s):
        for r in (1, 2, 3):
            gather(rx, s, r, rcv_c).wait_send()

    c_done(me)
    others(c_done)
    others(lambda d: comb_sp(d).wait_send())

    def pair_d(s):
        return copy(e1.at[s], d2.at[s], snd.at[s, 0], rcv_d2.at[s], (me, j2))

    def home(s):
        return copy(fin.at[s], ret.at[me], snd.at[s, 1], rcv_g.at[me], (s, j))

    swap_d(1).wait_recv()

    def d_pair(s):
        at = pl.ds(s, 1)
        e1[at] = (pd[2, at].astype(F32) + d1[1, at].astype(F32)).astype(BF16)
        pair_d(s).start()

    others(d_pair)
    d_pair(me)
    product(0)
    swap_d(0).wait_recv()

    def summed(s):
        at = pl.ds(s, 1)
        pair_d(s).wait_recv()
        return (pd[0, at].astype(F32) + d1[0, at].astype(F32) + d2[at].astype(F32)).astype(BF16)

    def d_home(s):
        fin[pl.ds(s, 1)] = summed(s)
        home(s).start()

    others(d_home)
    ret[pl.ds(me, 1)] = summed(me)
    others(lambda s: copy(fin.at[s], ret.at[s], snd.at[s, 1], rcv_g.at[s], (s, j)).wait_recv())
    moe = dot_tn(place, ret[...].reshape(slots, quarter))
    out_ref[...] = (stream.astype(F32) + moe).astype(BF16)

    for r in (1, 2, 3):
        swap_b(r).wait_send()
    swap_d(0).wait_send()
    swap_d(1).wait_send()
    pair_d(me).wait_send()

    def tail(s):
        pair_d(s).wait_send()
        home(s).wait_send()

    others(tail)


def body(
    n_sp, n_tp,
    query_wide, query_narrow, latent, rope_key, latent_norm_weight, broad_key_lift, broad_value_lift,
    slim_key_lift, slim_value_lift, out_wide, out_narrow, resid, ffn_gain, group_route, expert_pair,
    group_prob, expert_prob, gate_weight, up_weight, down_weight,
):
    tok, rank = latent.shape
    width = resid.shape[1]
    quarter = width // n_tp
    experts, _, ff = gate_weight.shape[1:]
    cap = max(2 * tok // n_sp, 16)
    kw, kn = broad_key_lift.shape[1], slim_key_lift.shape[1]
    heads_w, heads_n = kw // PLAIN_WIDE, kn // PLAIN_SLIM
    keys = n_sp * tok
    slots = n_sp * cap
    blk = min(slots, 256)

    freq = (1.0 / ROPE_BASE ** (np.arange(0, ROPE, 2).astype(np.float32) / np.float32(ROPE))).astype(np.float32)
    freq = np.tile(freq.astype(np.float64), LANES // (ROPE // 2))[None, :]
    base = (np.arange(n_sp) * tok)[:, None] * freq
    local = np.arange(tok)[:, None] * freq
    base_t = jnp.asarray(np.stack([np.cos(base), np.sin(base)]).astype(np.float32))
    local_t = jnp.asarray(np.stack([np.cos(local), np.sin(local)]).astype(np.float32))
    vm = pl.BlockSpec(memory_space=pltpu.VMEM)
    hb = pl.BlockSpec(memory_space=pl.ANY)
    dma = pltpu.SemaphoreType.DMA
    scratch = [
        pltpu.VMEM(query_wide.shape, BF16), pltpu.VMEM(query_narrow.shape, BF16),
        pltpu.VMEM(latent.shape, BF16), pltpu.VMEM(rope_key.shape[::-1], BF16),
        pltpu.VMEM((rank, 2 * kw + 2 * kn), BF16),
        pltpu.VMEM((kw + kn, width), BF16),
        pltpu.VMEM((tok, quarter), BF16),
        pltpu.VMEM((experts, width, 2 * ff), BF16),
        pltpu.VMEM((experts * ff, width), BF16),
        pltpu.VMEM((n_tp, tok // n_tp, rank + LANES), BF16),
        pltpu.VMEM((n_sp, n_tp, tok // n_tp, rank + LANES), BF16),
        pltpu.VMEM((keys, heads_w * 256 + heads_n * 128), BF16),
        pltpu.VMEM((keys, kw + kn), BF16),
        pltpu.VMEM((tok, kw + kn), BF16),
        pltpu.VMEM((4, tok, quarter), BF16),
        pltpu.VMEM((3, tok, quarter), BF16),
        pltpu.VMEM((n_sp, cap, quarter), BF16),
        pltpu.VMEM((n_sp, cap, LANES), BF16),
        pltpu.VMEM((n_sp, n_tp, cap, quarter), BF16),
        pltpu.VMEM((n_sp, cap, LANES), BF16),
        pltpu.VMEM((blk, width), BF16),
        pltpu.VMEM((slots, experts * ff), BF16),
        pltpu.VMEM((4, n_sp, cap, quarter), BF16),
        pltpu.VMEM((2, n_sp, cap, quarter), BF16),
        pltpu.VMEM((n_sp, cap, quarter), BF16),
        pltpu.VMEM((n_sp, cap, quarter), BF16),
        pltpu.VMEM((n_sp, cap, quarter), BF16),
        pltpu.VMEM((n_sp, cap, quarter), BF16),
        dma((13 + experts,)), dma((n_sp, 4)), dma((n_sp, 4)), dma((3,)), dma((3,)), dma((n_sp,)), dma((n_sp,)),
        dma((n_sp, 4)), dma((2,)), dma((2,)), dma((n_sp,)), dma((n_sp,)),
    ]
    call = pl.pallas_call(
        functools.partial(kernel, n_sp, n_tp, cap),
        out_shape=jax.ShapeDtypeStruct((tok, quarter), BF16),
        in_specs=[hb, hb, hb, hb, vm, hb, hb, hb, hb, hb, hb, hb, vm, vm, vm, vm, vm, vm, vm, hb, hb, hb],
        out_specs=vm,
        scratch_shapes=scratch,
        compiler_params=pltpu.CompilerParams(
            collective_id=0, has_side_effects=True, vmem_limit_bytes=67043328
        ),
    )
    return call(
        query_wide, query_narrow, latent, rope_key.T, latent_norm_weight[None, :], broad_key_lift,
        broad_value_lift, slim_key_lift, slim_value_lift, out_wide, out_narrow, resid, ffn_gain[None, :],
        group_route[None, :], expert_pair.T, group_prob[None, :], expert_prob.T, base_t, local_t, gate_weight, up_weight, down_weight,
    )


def solution(mesh):
    sizes = dict(mesh.shape)
    placed = (
        P("sp", "tp"), P("sp", "tp"), P("sp", None), P("sp", None), P(), P(None, "tp"), P(None, "tp"),
        P(None, "tp"), P(None, "tp"), P("tp", None), P("tp", None), P("sp", None), P(), P("sp"),
        P("sp", None), P("sp"), P("sp", None), P("sp", None, None, "tp"), P("sp", None, None, "tp"),
        P("sp", None, "tp", None),
    )
    return jax.shard_map(
        functools.partial(body, sizes["sp"], sizes["tp"]),
        mesh=mesh, in_specs=placed, out_specs=P("sp", "tp"), check_vma=False,
    )
```
